32 devices in a mesh: fs: 16 (over z, y, x), tp: 2 (over core).
Axes of the slice: x: 2, y: 2, z: 4, core: 2. Of those that a mesh axis runs over, the one named last changes fastest.
Arguments:
- normed_input: bfloat16 [8192, 4096], P('fs', 'tp'), may hold values from -6 to 6
- value_cotangent: bfloat16 [8192, 2048], P('fs', 'tp'), may hold values from -0.01171875 to 0.01171875
- mixer_output: bfloat16 [8192, 2048], P('fs', 'tp'), may hold values from -6 to 6
- output_cotangent: bfloat16 [8192, 4096], P('fs', 'tp'), may hold values from -0.015625 to 0.015625
- value_factor: bfloat16 [4096, 128], replicated, may hold values from -0.5 to 0.5
- output_factor: bfloat16 [2048, 128], replicated, may hold values from -0.5 to 0.5
- value_master: float32 [4096, 2048], P('fs', 'tp'), may hold values from -0.09375 to 0.09375
- value_moment: float32 [128, 2048], P(None, 'tp'), may hold values from -6 to 6
- value_second: float32 [128, 2048], P(None, 'tp'), may hold values from 0.0625 to 16, as said below
- output_master: float32 [2048, 4096], P('fs', 'tp'), may hold values from -0.125 to 0.125
- output_moment: float32 [128, 4096], P(None, 'tp'), may hold values from -6 to 6
- output_second: float32 [128, 4096], P(None, 'tp'), may hold values from 0.0625 to 16, as said below
Outputs:
- value_step: float32 [4096, 2048], P('fs', 'tp')
- value_new: float32 [4096, 2048], P('fs', 'tp')
- value_copy: bfloat16 [4096, 2048], P(None, 'tp')
- value_moment_new: float32 [128, 2048], P(None, 'tp')
- value_second_new: float32 [128, 2048], P(None, 'tp')
- output_step: float32 [2048, 4096], P('fs', 'tp')
- output_new: float32 [2048, 4096], P('fs', 'tp')
- output_copy: bfloat16 [2048, 4096], P(None, 'tp')
- output_moment_new: float32 [128, 4096], P(None, 'tp')
- output_second_new: float32 [128, 4096], P(None, 'tp')
The draws below stay inside these ranges and needn't reach their ends.
Inputs may be any that keep to these rules, and one draw needn't show every extreme that they name: `value_second`: positive, with a scale that differs between groups of columns. `output_second`: positive, with a scale that differs between groups of columns.
All inputs are finite; a program needn't handle non-finite values.
Results may differ from the reference program's by a relative error of at most 0.004.
Values may be sent and summed in bfloat16 or wider, within the bound.
A program may use at most 128 MiB of HBM per device.

```python
import math
import jax
import jax.numpy as jnp
from jax import lax

D = 4096
WIDTH = 2048
R = 128
TOK_DEV = 512
TOKENS = 8192
N_FS = 16
N_TP = 2


def second_draw(key, rows, columns):
    levels = jnp.exp(jax.random.uniform(jax.random.fold_in(key, 11), (rows, columns), jnp.float32, math.log(0.25), math.log(4.0)))
    groups = jnp.exp(jax.random.uniform(jax.random.fold_in(key, 12), (16,), jnp.float32, math.log(0.25), math.log(4.0)))
    return levels * jnp.repeat(groups, columns // 16)[None, :]


def draw_value_second(key, part):
    return second_draw(jax.random.fold_in(key, 1), R, WIDTH)


def draw_output_second(key, part):
    return second_draw(jax.random.fold_in(key, 2), R, D)


def strengthened(array, rng, source, target, parts, factor):
    def block_of(axis_at):
        return (jnp.arange(array.shape[axis_at]) // (array.shape[axis_at] // parts)).reshape((-1,) + (1,) * (array.ndim - 1 - axis_at))

    near = jax.random.permutation(rng, parts)[block_of(target)]
    other_side = (block_of(target) + parts // 2) % parts
    return jnp.where((block_of(source) == near) | (block_of(source) == other_side), factor * array, array)


def block_levels(own_key, extent, split, least, top_value):
    def one(axis_at, parts):
        draws = jax.random.uniform(jax.random.fold_in(jax.random.fold_in(own_key, 6), axis_at), (parts,), jnp.float32, least / len(split), top_value / len(split))
        return jnp.repeat(jnp.exp(draws), extent[axis_at] // parts).reshape((-1,) + (1,) * (len(extent) - axis_at - 1))

    factor_of = one(*split[0])
    for cut in split[1:]:
        factor_of = factor_of * one(*cut)
    return factor_of


def noise(key, extent, width, reach, pieces=(), dtype=jnp.bfloat16):
    result = width * jax.random.normal(key, extent, jnp.float32)
    if pieces:
        result = result * block_levels(key, extent, pieces, -0.22, 0.18)
    return jnp.clip(result, -reach, reach).astype(dtype)


def gaussian_with(key, dims, scale, bound, shards, heavy, held_as=jnp.bfloat16):
    array = scale * jax.random.normal(key, dims, jnp.float32)
    if shards:
        array = array * block_levels(key, dims, shards, -0.22, 0.18)
    return jnp.clip(strengthened(array, jax.random.fold_in(key, 3), *heavy), -bound, bound).astype(held_as)


def setup_inputs(seed: int = 0) -> dict:
    streams_of = jax.random.split(jax.random.key(seed), 13)
    return {
        "normed_input": gaussian_with(streams_of[0], (TOKENS, D), 1.0, 6.0, ((0, 16), (1, 2)), (0, 1, 16, 2.0)),
        "value_cotangent": noise(streams_of[1], (TOKENS, WIDTH), ((R / (D * TOK_DEV * N_FS)) ** 0.5), 0.01171875, ((0, 16), (1, 2))),
        "mixer_output": noise(streams_of[2], (TOKENS, WIDTH), 1.0, 6.0, ((0, 16), (1, 2))),
        "output_cotangent": noise(streams_of[3], (TOKENS, D), ((R / (WIDTH * TOK_DEV * N_FS)) ** 0.5), 0.015625, ((0, 16), (1, 2))),
        "value_factor": noise(streams_of[4], (D, R), R ** -0.5, 0.5),
        "output_factor": noise(streams_of[5], (WIDTH, R), R ** -0.5, 0.5),
        "value_master": noise(streams_of[6], (D, WIDTH), D ** -0.5, 0.09375, ((0, 16), (1, 2)), jnp.float32),
        "value_moment": noise(streams_of[7], (R, WIDTH), 1.0, 6.0, ((1, 2),), jnp.float32),
        "value_second": draw_value_second(jax.random.fold_in(streams_of[12], 71), 0),
        "output_master": noise(streams_of[9], (WIDTH, D), WIDTH ** -0.5, 0.125, ((0, 16), (1, 2)), jnp.float32),
        "output_moment": noise(streams_of[10], (R, D), 1.0, 6.0, ((1, 2),), jnp.float32),
        "output_second": draw_output_second(jax.random.fold_in(streams_of[12], 71), 0),
    }


BETA_ONE = 0.8
BETA_TWO = 0.9
EPSILON = 1e-08
STEP_RATE = 0.005
FLOOR = 0.25

def moments(first, second, projected):
    first_new = BETA_ONE * first + (1.0 - BETA_ONE) * projected
    second_new = BETA_TWO * second + (1.0 - BETA_TWO) * projected * projected
    normalized = first_new / (jnp.sqrt(second_new) + EPSILON)
    return (first_new, second_new, normalized)

def reference(normed_input, value_cotangent, mixer_output, output_cotangent, value_factor, output_factor, value_master, value_moment, value_second, output_master, output_moment, output_second):
    highest = lax.Precision.HIGHEST
    input_reduced = jnp.dot(normed_input.astype(jnp.float32), value_factor.astype(jnp.float32), precision=highest)
    value_projected = jnp.dot(input_reduced.T, value_cotangent.astype(jnp.float32), precision=highest)
    split_cols = WIDTH // N_TP
    mixer_blocks = mixer_output.astype(jnp.float32).reshape(TOKENS, N_TP, split_cols)
    factor_blocks = output_factor.astype(jnp.float32).reshape(N_TP, split_cols, R)
    partials = jnp.einsum('tnc,ncr->ntr', mixer_blocks, factor_blocks, precision=highest).astype(jnp.bfloat16)
    partials = lax.optimization_barrier(partials)
    mixer_reduced = lax.optimization_barrier(jnp.sum(partials.astype(jnp.float32), axis=0)).astype(jnp.bfloat16)
    output_projected = jnp.dot(mixer_reduced.astype(jnp.float32).T, output_cotangent.astype(jnp.float32), precision=highest)
    value_moment_new, value_second_new, value_norm = moments(value_moment, value_second, value_projected)
    output_moment_new, output_second_new, output_norm = moments(output_moment, output_second, output_projected)
    value_scale = lax.rsqrt(jnp.mean(value_norm * value_norm) + FLOOR)
    output_scale = lax.rsqrt(jnp.mean(output_norm * output_norm) + FLOOR)
    value_step = value_scale * jnp.dot(value_factor.astype(jnp.float32), value_norm, precision=highest)
    output_step = output_scale * jnp.dot(output_factor.astype(jnp.float32), output_norm, precision=highest)
    value_new = value_master - STEP_RATE * value_step
    output_new = output_master - STEP_RATE * output_step
    return (value_step, value_new, value_new.astype(jnp.bfloat16), value_moment_new, value_second_new, output_step, output_new, output_new.astype(jnp.bfloat16), output_moment_new, output_second_new)
```

```python
import functools

import jax
import jax.numpy as jnp
from jax import lax
from jax.experimental import pallas as pl
from jax.experimental.pallas import tpu as pltpu
from jax.sharding import PartitionSpec as P

BETA_ONE = 0.8
BETA_TWO = 0.9
EPSILON = 1e-08
STEP_RATE = 0.005
FLOOR = 0.25

MESH = pl.DeviceIdType.MESH
PIECES = 8
UP, DOWN, ACROSS_A, ACROSS_B = range(4)
GROUPS = (
    (0, 0, 4, True, (ACROSS_A, ACROSS_B)),
    (1, 0, 4, True, (ACROSS_B, ACROSS_A)),
    (0, 4, 7, True, (ACROSS_B, ACROSS_A)),
    (1, 4, 7, True, (ACROSS_A, ACROSS_B)),
    (0, 7, 8, False, (ACROSS_A, ACROSS_B)),
    (1, 7, 8, False, (ACROSS_B, ACROSS_A)),
)


def transfer_kernel(
    n_fs,
    n_tp,
    input_ref,
    mixer_ref,
    value_cot_ref,
    output_cot_ref,
    value_own,
    output_own,
    value_all,
    output_all,
    value_sum,
    output_sum,
    near_in,
    near_mix,
    value_part,
    output_part,
    value_recv,
    output_recv,
    gather_send,
    gather_recv,
    local_sem,
    near_send,
    near_recv,
    scatter_send,
    scatter_recv,
    total_send,
    total_recv,
):
    me = lax.axis_index("fs")
    column = lax.axis_index("tp")
    n_a = 2 if n_fs % 2 == 0 else 1
    n_b = 2 if n_fs % 4 == 0 else 1
    plane = n_a * n_b
    n_z = n_fs // plane
    here_a = lax.rem(me, n_a)
    here_b = lax.rem(me // n_a, n_b)
    here_z = me // plane
    owns = (value_own, output_own)
    alls = (value_all, output_all)

    def index_of(z, flip_a, flip_b):
        a = n_a - 1 - here_a if flip_a else here_a
        b = n_b - 1 - here_b if flip_b else here_b
        return z * plane + b * n_a + a

    targets = {
        UP: me + plane,
        DOWN: me - plane,
        ACROSS_A: index_of(here_z, True, False),
        ACROSS_B: index_of(here_z, False, True),
    }
    can = {UP: here_z < n_z - 1, DOWN: here_z > 0, ACROSS_A: n_a > 1, ACROSS_B: n_b > 1}

    def copy_of(way, source, group, own):
        array, low, high, _, _ = GROUPS[group]
        there = alls[array].at[source, low:high]
        return pltpu.make_async_remote_copy(
            src_ref=owns[array].at[low:high] if own else there,
            dst_ref=there,
            send_sem=gather_send.at[way, source, group],
            recv_sem=gather_recv.at[source, group],
            device_id={"fs": targets[way]},
            device_id_type=MESH,
        )

    def guarded(condition, action):
        if isinstance(condition, bool):
            if condition:
                action()
        else:
            pl.when(condition)(action)

    sent = []

    def send(way, source, group, own=False, valid=True):
        def begin():
            copy_of(way, source, group, own).start()

        def finish():
            copy_of(way, source, group, own).wait_send()

        condition = can[way]
        if valid is not True:
            condition = jnp.logical_and(condition, valid) if condition is not True else valid
        guarded(condition, begin)
        sent.append((condition, finish))

    def take(way, source, group):
        copy_of(way, source, group, False).wait_recv()

    def flips(axis):
        return axis == ACROSS_A, axis == ACROSS_B

    z_groups = [g for g in range(len(GROUPS)) if GROUPS[g][3]]
    plane_groups = [g for g in range(len(GROUPS)) if not GROUPS[g][3]]

    near = []
    for k in range(1, n_tp):
        for i, (src, dst) in enumerate(((input_ref, near_in), (mixer_ref, near_mix))):
            near.append(
                pltpu.make_async_remote_copy(
                    src_ref=src,
                    dst_ref=dst.at[k - 1],
                    send_sem=near_send.at[k - 1, i],
                    recv_sem=near_recv.at[k - 1, i],
                    device_id={"tp": lax.rem(column + k, n_tp)},
                    device_id_type=MESH,
                )
            )
    for copy in near:
        copy.start()

    for group in z_groups + plane_groups:
        for way in (UP, DOWN, ACROSS_A, ACROSS_B):
            send(way, me, group, own=True)
    keep = [
        pltpu.make_async_copy(owns[i], alls[i].at[me], local_sem.at[i]) for i in range(2)
    ]
    for copy in keep:
        copy.start()

    for copy in near:
        copy.wait()
    input_total = input_ref[...].astype(jnp.float32)
    mixer_total = mixer_ref[...].astype(jnp.float32)
    for k in range(n_tp - 1):
        input_total += near_in[k].astype(jnp.float32)
        mixer_total += near_mix[k].astype(jnp.float32)
    across = (((0,), (0,)), ((), ()))
    rows = value_part.shape[1]
    scatter = []
    for i, (left, right, part, recv) in enumerate(
        (
            (input_total.astype(jnp.bfloat16), value_cot_ref, value_part, value_recv),
            (mixer_total.astype(jnp.bfloat16), output_cot_ref, output_part, output_recv),
        )
    ):
        width = right.shape[1]
        tile = 512 if width % 512 == 0 else width
        for c in range(width // tile):
            cols = slice(c * tile, (c + 1) * tile)
            product = lax.dot_general(
                left, right[:, cols], across, preferred_element_type=jnp.float32
            )
            for s in range(n_fs):
                part[s, :, cols] = product[s * rows : (s + 1) * rows]
        for k in range(1, n_fs):
            there = lax.rem(me + k, n_fs)
            copy = pltpu.make_async_remote_copy(
                src_ref=part.at[there],
                dst_ref=recv.at[k],
                send_sem=scatter_send.at[i, k],
                recv_sem=scatter_recv.at[i, k],
                device_id={"fs": there},
                device_id_type=MESH,
            )
            copy.start()
            scatter.append(copy)

    def plane_round():
        for group in plane_groups:
            first, second = GROUPS[group][4]
            if can[first]:
                source = index_of(here_z, *flips(first))
                take(first, source, group)
                for way in (second, UP, DOWN):
                    send(way, source, group)
        for group in plane_groups:
            first, second = GROUPS[group][4]
            if can[second]:
                for both in (False, True):
                    if both and not can[first]:
                        continue
                    source = index_of(
                        here_z,
                        second == ACROSS_A or (both and first == ACROSS_A),
                        second == ACROSS_B or (both and first == ACROSS_B),
                    )
                    take(second, source, group)
                    for way in (UP, DOWN):
                        send(way, source, group)

    def z_round(d):
        for sign, onward in ((-1, UP), (1, DOWN)):
            z = here_z + sign * d
            valid = z >= 0 if sign < 0 else z <= n_z - 1

            for group in z_groups:
                source = index_of(z, False, False)

                @pl.when(valid)
                def _(group=group, source=source):
                    take(DOWN if onward == UP else UP, source, group)

                send(onward, source, group, valid=valid)
                for way in GROUPS[group][4]:
                    send(way, source, group, valid=valid)
            for group in plane_groups:
                for flip_a in range(n_a):
                    for flip_b in range(n_b):
                        source = index_of(z, flip_a == 1, flip_b == 1)

                        @pl.when(valid)
                        def _(group=group, source=source):
                            take(DOWN if onward == UP else UP, source, group)

                        send(onward, source, group, valid=valid)

    def column_round(d):
        for sign in (-1, 1):
            if d == 0 and sign == 1:
                continue
            z = here_z + sign * d
            valid = True if d == 0 else (z >= 0 if sign < 0 else z <= n_z - 1)
            for group in z_groups:
                first, second = GROUPS[group][4]
                if not can[first]:
                    continue
                source = index_of(z, *flips(first))
                guarded(valid, functools.partial(take, first, source, group))
                send(second, source, group, valid=valid)

    totals = []

    def share_totals():
        for copy in scatter:
            copy.wait_recv()
        for i, (part, recv, out) in enumerate(
            ((value_part, value_recv, value_sum), (output_part, output_recv, output_sum))
        ):
            total = part[me]
            for k in range(1, n_fs):
                total += recv[k]
            out[me] = total
            for k in range(1, n_fs):
                there = lax.rem(me + k, n_fs)
                copy = pltpu.make_async_remote_copy(
                    src_ref=out.at[me],
                    dst_ref=out.at[me],
                    send_sem=total_send.at[i, k],
                    recv_sem=total_recv.at[i, k],
                    device_id={"fs": there},
                    device_id_type=MESH,
                )
                copy.start()
                source = lax.rem(me + n_fs - k, n_fs)
                arriving = pltpu.make_async_remote_copy(
                    src_ref=out.at[source],
                    dst_ref=out.at[source],
                    send_sem=total_send.at[i, k],
                    recv_sem=total_recv.at[i, k],
                    device_id={"fs": there},
                    device_id_type=MESH,
                )
                totals.append((copy, arriving))

    plane_round()
    column_round(0)
    for d in range(1, n_z):
        z_round(d)
        if d == 1:
            share_totals()
        column_round(d)
    if n_z == 1:
        share_totals()

    for group in z_groups:
        first, second = GROUPS[group][4]
        if can[second]:
            for z in range(n_z):
                for both in (False, True):
                    if both and not can[first]:
                        continue
                    source = index_of(
                        z,
                        second == ACROSS_A or (both and first == ACROSS_A),
                        second == ACROSS_B or (both and first == ACROSS_B),
                    )
                    take(second, source, group)
    for copy, arriving in totals:
        copy.wait_send()
        arriving.wait_recv()
    for copy in scatter:
        copy.wait_send()
    for condition, finish in sent:
        guarded(condition, finish)
    for copy in keep:
        copy.wait()


def transfers(n_fs, n_tp, inputs, mixer, value_cot, output_cot, value_own, output_own, rank):
    f32, bf16 = jnp.float32, jnp.bfloat16
    rows = rank // n_fs
    value_cols, output_cols = value_cot.shape[1], output_cot.shape[1]
    tokens = inputs.shape[0]
    vmem = pl.BlockSpec(memory_space=pltpu.VMEM)
    hbm = pl.BlockSpec(memory_space=pltpu.HBM)
    groups = len(GROUPS)
    dma = pltpu.SemaphoreType.DMA
    return pl.pallas_call(
        functools.partial(transfer_kernel, n_fs, n_tp),
        out_shape=(
            jax.ShapeDtypeStruct((n_fs,) + value_own.shape, bf16),
            jax.ShapeDtypeStruct((n_fs,) + output_own.shape, bf16),
            jax.ShapeDtypeStruct((n_fs, rows, value_cols), f32),
            jax.ShapeDtypeStruct((n_fs, rows, output_cols), f32),
        ),
        in_specs=[vmem] * 6,
        out_specs=(hbm, hbm, vmem, vmem),
        scratch_shapes=[
            pltpu.VMEM((max(n_tp - 1, 1), tokens, rank), bf16),
            pltpu.VMEM((max(n_tp - 1, 1), tokens, rank), bf16),
            pltpu.VMEM((n_fs, rows, value_cols), f32),
            pltpu.VMEM((n_fs, rows, output_cols), f32),
            pltpu.VMEM((n_fs, rows, value_cols), f32),
            pltpu.VMEM((n_fs, rows, output_cols), f32),
            dma((4, n_fs, groups)),
            dma((n_fs, groups)),
            dma((2,)),
            dma((max(n_tp - 1, 1), 2)),
            dma((max(n_tp - 1, 1), 2)),
            dma((2, n_fs)),
            dma((2, n_fs)),
            dma((2, n_fs)),
            dma((2, n_fs)),
        ],
        compiler_params=pltpu.CompilerParams(has_side_effects=True),
    )(inputs, mixer, value_cot, output_cot, value_own, output_own)


def moments(first, second, projected):
    first_new = BETA_ONE * first + (1.0 - BETA_ONE) * projected
    second_new = BETA_TWO * second + (1.0 - BETA_TWO) * projected * projected
    normalized = first_new / (jnp.sqrt(second_new) + EPSILON)
    return (first_new, second_new, normalized)


def halves(norm):
    high = lax.reduce_precision(norm, 8, 7)
    low = norm - high
    return jnp.concatenate([high, low], axis=0).astype(jnp.bfloat16)


def per_device(
    n_fs,
    n_tp,
    normed_input,
    value_cotangent,
    mixer_output,
    output_cotangent,
    value_factor,
    output_factor,
    value_master,
    value_moment,
    value_second,
    output_master,
    output_moment,
    output_second,
):
    row_index = lax.axis_index("fs")
    column_index = lax.axis_index("tp")
    rank = value_factor.shape[1]
    value_rows, value_cols = value_master.shape
    output_rows, output_cols = output_master.shape
    feature_cols = normed_input.shape[1]
    factor_features = lax.dynamic_slice_in_dim(
        value_factor, column_index * feature_cols, feature_cols, 0
    )
    input_partial = jnp.dot(
        normed_input, factor_features, preferred_element_type=jnp.float32
    ).astype(jnp.bfloat16)
    head_cols = mixer_output.shape[1]
    factor_heads = lax.dynamic_slice_in_dim(output_factor, column_index * head_cols, head_cols, 0)
    mixer_partial = jnp.dot(
        mixer_output, factor_heads, preferred_element_type=jnp.float32
    ).astype(jnp.bfloat16)

    value_all, output_all, value_sum, output_sum = transfers(
        n_fs,
        n_tp,
        input_partial,
        mixer_partial,
        value_cotangent,
        output_cotangent,
        value_master.astype(jnp.bfloat16).reshape(PIECES, value_rows // PIECES, value_cols),
        output_master.astype(jnp.bfloat16).reshape(PIECES, output_rows // PIECES, output_cols),
        rank,
    )
    value_moment_new, value_second_new, value_norm = moments(
        value_moment, value_second, value_sum.reshape(rank, value_cols)
    )
    output_moment_new, output_second_new, output_norm = moments(
        output_moment, output_second, output_sum.reshape(rank, output_cols)
    )
    value_total, output_total = lax.psum(
        (jnp.sum(value_norm * value_norm), jnp.sum(output_norm * output_norm)), "tp"
    )
    value_scale = lax.rsqrt(value_total / (rank * value_cols * n_tp) + FLOOR)
    output_scale = lax.rsqrt(output_total / (rank * output_cols * n_tp) + FLOOR)

    def update(factor, norm, scale, master, gathered):
        pair = halves(norm)
        double = jnp.concatenate([factor, factor], axis=1)
        rows = master.shape[0]
        double_here = lax.dynamic_slice_in_dim(double, row_index * rows, rows, 0)
        step = scale * jnp.dot(double_here, pair, preferred_element_type=jnp.float32)
        new = master - STEP_RATE * step
        full = jnp.dot(double, pair, preferred_element_type=jnp.float32)
        flat = gathered.reshape(n_fs * rows, master.shape[1]).astype(jnp.float32)
        copy = (flat - (STEP_RATE * scale) * full).astype(jnp.bfloat16)
        return step, new, copy

    value_step, value_new, value_copy = update(
        value_factor, value_norm, value_scale, value_master, value_all
    )
    output_step, output_new, output_copy = update(
        output_factor, output_norm, output_scale, output_master, output_all
    )
    return (
        value_step,
        value_new,
        value_copy,
        value_moment_new,
        value_second_new,
        output_step,
        output_new,
        output_copy,
        output_moment_new,
        output_second_new,
    )


def solution(mesh):
    return jax.shard_map(
        functools.partial(per_device, mesh.shape["fs"], mesh.shape["tp"]),
        mesh=mesh,
        in_specs=(
            P("fs", "tp"),
            P("fs", "tp"),
            P("fs", "tp"),
            P("fs", "tp"),
            P(),
            P(),
            P("fs", "tp"),
            P(None, "tp"),
            P(None, "tp"),
            P("fs", "tp"),
            P(None, "tp"),
            P(None, "tp"),
        ),
        out_specs=(
            P("fs", "tp"),
            P("fs", "tp"),
            P(None, "tp"),
            P(None, "tp"),
            P(None, "tp"),
            P("fs", "tp"),
            P("fs", "tp"),
            P(None, "tp"),
            P(None, "tp"),
            P(None, "tp"),
        ),
        check_vma=False,
    )
```
